32 devices in a mesh: fs: 4 (over z), rep: 4 (over y, x), tp: 2 (over core).
Axes of the slice: x: 2, y: 2, z: 4, core: 2. Of those that a mesh axis runs over, the one named last changes fastest.
Arguments:
- saved_input: bfloat16 [16384, 2048], P(('fs', 'rep')), may hold values from -500 to 500
- query_cotangent: bfloat16 [16384, 2048], P(('fs', 'rep'), 'tp'), may hold values from -0.014038086 to 0.014038086
- key_cotangent: bfloat16 [16384, 512], P(('fs', 'rep'), 'tp'), may hold values from -0.014038086 to 0.014038086
- query_weight: float32 [2048, 2048], P('fs', 'tp'), may hold values from -45 to 45
- key_weight: float32 [2048, 512], P('fs', 'tp'), may hold values from -45 to 45
- query_moment: float32 [2048, 2048], P('fs', 'tp'), may hold values from -45 to 45
- key_moment: float32 [2048, 512], P('fs', 'tp'), may hold values from -45 to 45
- query_row_root: bfloat16 [2048, 2048], P('fs'), may hold values from -1 to 3, as said below
- key_row_root: bfloat16 [2048, 2048], P('fs'), may hold values from -1 to 3, as said below
- query_head_root: bfloat16 [32, 64, 64], P('tp'), may hold values from -1 to 3, as said below
- key_head_root: bfloat16 [8, 64, 64], P('tp'), may hold values from -1 to 3, as said below
- query_head_stat: float32 [32, 64, 64], P('tp'), may hold values from -26 to 27, as said below
- key_head_stat: float32 [8, 64, 64], P('tp'), may hold values from -26 to 27, as said below
Outputs:
- query_step: float32 [2048, 2048], P('fs', 'tp')
- key_step: float32 [2048, 512], P('fs', 'tp')
- query_next: float32 [2048, 2048], P('fs', 'tp')
- key_next: float32 [2048, 512], P('fs', 'tp')
- query_copy: bfloat16 [2048, 2048], P(None, 'tp')
- key_copy: bfloat16 [2048, 512], P(None, 'tp')
- query_moment_next: float32 [2048, 2048], P('fs', 'tp')
- key_moment_next: float32 [2048, 512], P('fs', 'tp')
- query_stat_next: float32 [32, 64, 64], P('tp')
- key_stat_next: float32 [8, 64, 64], P('tp')
The draws below stay inside these ranges and needn't reach their ends.
Inputs may be any that keep to these rules, and one draw needn't show every extreme that they name: `query_row_root`: symmetric. `key_row_root`: symmetric. `query_head_root`: each head's matrix is symmetric. `key_head_root`: each head's matrix is symmetric. `query_head_stat`: each head's matrix is symmetric. `key_head_stat`: each head's matrix is symmetric.
All inputs are finite; a program needn't handle non-finite values.
Results may differ from the reference program's by a relative error of at most 0.0018.
The reference program's roundings to bfloat16 on the way count: a program that leaves them out, or rounds other values in their place, can miss the bound.
Values may be sent and summed in bfloat16 or wider, within the bound.
A program may use at most 128 MiB of HBM per device.

```python
import math
import jax
import jax.numpy as jnp
from jax import lax

D = 2048
HEAD_DIM = 64
QHEADS = 32
KVHEADS = 8
TOKENS = 16384
QW = 2048
KW = 512


def rising_scale(length):
    return jnp.exp(jnp.linspace(math.log(0.3), math.log(3.0), length)).astype(jnp.float32)


def column_rise(length):
    return jnp.exp(jnp.linspace(0.0, math.log(10.0), length)).astype(jnp.float32)


def bounded_entries(rng_key, shape):
    return jax.random.truncated_normal(rng_key, -5.0, 5.0, shape, jnp.float32)


def matrix_draw(key, marker, row_total, col_total):
    first_key, second_key = jax.random.split(jax.random.fold_in(key, marker))
    entries = bounded_entries(first_key, (row_total, col_total))
    col_scale = jnp.exp(jax.random.uniform(second_key, (1, col_total), jnp.float32, math.log(0.3), math.log(3.0)))
    return entries * rising_scale(row_total)[:, None] * col_scale


def root_draw(key, marker, count_mats, order):
    first_key, second_key = jax.random.split(jax.random.fold_in(key, marker))
    diagonal = jnp.exp(jax.random.uniform(first_key, (count_mats, order), jnp.float32, math.log(0.5), math.log(2.0)))
    off_diagonal = bounded_entries(second_key, (count_mats, order, order)) * (0.7 / math.sqrt(order))
    symmetric = 0.5 * (off_diagonal + jnp.swapaxes(off_diagonal, 1, 2))
    identity = jnp.eye(order, dtype=jnp.float32)[None]
    return symmetric * (1.0 - identity) + diagonal[:, :, None] * identity


def stat_draw(key, marker, count_mats):
    factor = bounded_entries(jax.random.fold_in(key, marker), (count_mats, HEAD_DIM, HEAD_DIM))
    gram = jnp.einsum('hde,hfe->hdf', factor, factor, precision=jax.lax.Precision.HIGHEST) / HEAD_DIM
    return gram + 0.6 * jnp.eye(HEAD_DIM, dtype=jnp.float32)[None]


def draw_saved_input(key, part):
    first_key, second_key = jax.random.split(jax.random.fold_in(key, 101))
    entries = bounded_entries(first_key, (TOKENS, D))
    token_scale = jnp.exp(jax.random.uniform(second_key, (TOKENS, 1), jnp.float32, 0.0, math.log(10.0)))
    return (entries * token_scale * column_rise(D)[None, :]).astype(jnp.bfloat16)


def draw_query_weight(key, part):
    return matrix_draw(key, 201, D, QHEADS * HEAD_DIM)


def draw_key_weight(key, part):
    return matrix_draw(key, 202, D, KVHEADS * HEAD_DIM)


def draw_query_moment(key, part):
    return matrix_draw(key, 203, D, QHEADS * HEAD_DIM)


def draw_key_moment(key, part):
    return matrix_draw(key, 204, D, KVHEADS * HEAD_DIM)


def draw_query_row_root(key, part):
    return root_draw(key, 301, 1, D)[0].astype(jnp.bfloat16)


def draw_key_row_root(key, part):
    return root_draw(key, 302, 1, D)[0].astype(jnp.bfloat16)


def draw_query_head_root(key, part):
    return root_draw(key, 303, QHEADS, HEAD_DIM).astype(jnp.bfloat16)


def draw_key_head_root(key, part):
    return root_draw(key, 304, KVHEADS, HEAD_DIM).astype(jnp.bfloat16)


def draw_query_head_stat(key, part):
    return stat_draw(key, 401, QHEADS)


def draw_key_head_stat(key, part):
    return stat_draw(key, 402, KVHEADS)


def block_levels(rng, extent, cuts, smallest, largest):
    loudness = 1.0
    for axis_at, parts in cuts:
        heights = jax.random.uniform(jax.random.fold_in(jax.random.fold_in(rng, 6), axis_at), (parts,), jnp.float32, smallest / len(cuts), largest / len(cuts))
        loudness = loudness * jnp.repeat(jnp.exp(heights), extent[axis_at] // parts).reshape((-1,) + (1,) * (len(extent) - 1 - axis_at))
    return loudness


def normal_values(key, extent, spread, most, cuts=(), kind=jnp.bfloat16):
    factor_of = block_levels(key, extent, cuts, -0.22, 0.18) if cuts else 1.0
    array = jax.random.normal(key, extent, jnp.float32) * spread * factor_of
    return jnp.minimum(jnp.maximum(array, -most), most).astype(kind)


def setup_inputs(seed: int = 0) -> dict:
    seeds = jax.random.split(jax.random.key(seed), 14)
    saved_input = draw_saved_input(jax.random.fold_in(seeds[13], 71), 0)
    query_cotangent = normal_values(seeds[1], (TOKENS, QW), (0.3 / TOKENS ** 0.5), 0.014038086, ((0, 16), (1, 2)))
    key_cotangent = normal_values(seeds[2], (TOKENS, KW), (0.3 / TOKENS ** 0.5), 0.014038086, ((0, 16), (1, 2)))
    query_weight = draw_query_weight(jax.random.fold_in(seeds[13], 71), 0)
    key_weight = draw_key_weight(jax.random.fold_in(seeds[13], 71), 0)
    query_moment = draw_query_moment(jax.random.fold_in(seeds[13], 71), 0)
    key_moment = draw_key_moment(jax.random.fold_in(seeds[13], 71), 0)
    query_row_root = draw_query_row_root(jax.random.fold_in(seeds[13], 71), 0)
    key_row_root = draw_key_row_root(jax.random.fold_in(seeds[13], 71), 0)
    query_head_root = draw_query_head_root(jax.random.fold_in(seeds[13], 71), 0)
    key_head_root = draw_key_head_root(jax.random.fold_in(seeds[13], 71), 0)
    query_head_stat = draw_query_head_stat(jax.random.fold_in(seeds[13], 71), 0)
    key_head_stat = draw_key_head_stat(jax.random.fold_in(seeds[13], 71), 0)
    return dict(saved_input=saved_input, query_cotangent=query_cotangent, key_cotangent=key_cotangent, query_weight=query_weight, key_weight=key_weight, query_moment=query_moment, key_moment=key_moment, query_row_root=query_row_root, key_row_root=key_row_root, query_head_root=query_head_root, key_head_root=key_head_root, query_head_stat=query_head_stat, key_head_stat=key_head_stat)


MOMENT_DECAY = 0.8
STAT_DECAY = 0.5
LEARN_RATE = 0.1
EPSILON = 1e-06

def update(gradient, weight, moment, stat, row_root, head_root):
    row_total = gradient.shape[0]
    head_count = head_root.shape[0]
    rounded = lax.optimization_barrier(gradient.astype(jnp.bfloat16)).astype(jnp.float32)
    shaped = rounded.reshape(row_total, head_count, HEAD_DIM)
    gram = jnp.einsum('rhd,rhe->hde', shaped, shaped)
    stat_next = STAT_DECAY * stat + (1.0 - STAT_DECAY) * gram / D
    rightward = jnp.einsum('rhd,hde->rhe', shaped, head_root.astype(jnp.float32))
    rightward = rightward.reshape(row_total, head_count * HEAD_DIM).astype(jnp.bfloat16)
    preconditioned = jnp.dot(row_root, rightward, preferred_element_type=jnp.float32)
    moment_next = MOMENT_DECAY * moment + (1.0 - MOMENT_DECAY) * preconditioned
    trust_ratio = jnp.sqrt(jnp.sum(weight * weight)) / jnp.sqrt(jnp.sum(moment_next * moment_next) + EPSILON)
    update_step = LEARN_RATE * trust_ratio * moment_next
    weight_next = weight - update_step
    return (update_step, weight_next, weight_next.astype(jnp.bfloat16), moment_next, stat_next)

def token_sum(saved_input, cotangent):
    return lax.dot_general(saved_input, cotangent, (((0,), (0,)), ((), ())), preferred_element_type=jnp.float32)

def reference(saved_input, query_cotangent, key_cotangent, query_weight, key_weight, query_moment, key_moment, query_row_root, key_row_root, query_head_root, key_head_root, query_head_stat, key_head_stat):
    query_out = update(token_sum(saved_input, query_cotangent), query_weight, query_moment, query_head_stat, query_row_root, query_head_root)
    key_out = update(token_sum(saved_input, key_cotangent), key_weight, key_moment, key_head_stat, key_row_root, key_head_root)
    return (query_out[0], key_out[0], query_out[1], key_out[1], query_out[2], key_out[2], query_out[3], key_out[3], query_out[4], key_out[4])
```

```python
import functools

import jax
import jax.numpy as jnp
from jax import lax
from jax.experimental import pallas as pl
from jax.experimental.pallas import tpu as pltpu
from jax.sharding import PartitionSpec as P

HEAD_DIM = 64
LANES = 128

MOMENT_DECAY = 0.8
STAT_DECAY = 0.5
LEARN_RATE = 0.1
EPSILON = 1e-06


def log2(n):
    return n.bit_length() - 1


class Cube:
    def __init__(self, fs, rep, block):
        self.fs, self.rep, self.block = fs, rep, block
        self.low, self.high = log2(rep), log2(fs)
        self.dims = self.low + self.high
        f, r = lax.axis_index("fs"), lax.axis_index("rep")
        self.f, self.r = f, r
        self.bits = [(r // 2**k) % 2 for k in range(self.low)]
        self.bits += [(f // 2**k) % 2 for k in range(self.high)]
        self.me = f * rep + r

    def partner(self, bit):
        flip = 1 - 2 * self.bits[bit]
        if bit < self.low:
            return {"rep": self.r + flip * 2**bit}
        return {"fs": self.f + flip * 2 ** (bit - self.low)}

    def rows(self, free, j, flipped=None):
        index = self.me
        for k, bit in enumerate(free):
            index = index + ((j // 2**k) % 2) * ((1 - 2 * self.bits[bit]) * 2**bit)
        if flipped is not None:
            index = index + (1 - 2 * self.bits[flipped]) * 2**flipped
        return pl.ds(pl.multiple_of(index * self.block, self.block), self.block)

    def barrier(self):
        barrier = pltpu.get_barrier_semaphore()
        for bit in range(self.dims):
            pl.semaphore_signal(
                barrier, inc=1, device_id=self.partner(bit), device_id_type=pl.DeviceIdType.MESH
            )
        pl.semaphore_wait(barrier, self.dims)


def each(start, stop, body):
    if stop - start <= 8:
        for j in range(start, stop):
            body(j)
    else:
        lax.fori_loop(start, stop, lambda j, _: (body(j), 0)[1], 0)


def orders(low, high):
    rep_bits, fs_bits = list(range(low)), list(range(low, low + high))
    near, far = fs_bits[:1], fs_bits[1:]
    return {
        "a": rep_bits + near + far,
        "b": rep_bits[::-1] + near + far,
        "c": near + rep_bits + far,
        "d": near + rep_bits[::-1] + far,
    }


KINDS = "abcababdab"


def drain(ref, sem):
    pltpu.make_async_copy(ref, ref, sem).wait()


def gather_sends(cube, held, chunk, order, step, send_sem, recv_sem, known_plane):
    bit = order[step]
    free = sorted(order[:step])
    start = 0
    if known_plane and bit < cube.low:
        start = 2 ** len([b for b in free if b < cube.low])

    def send(j):
        rows = cube.rows(free, j)
        pltpu.make_async_remote_copy(
            src_ref=held.at[chunk, rows],
            dst_ref=held.at[chunk, rows],
            send_sem=send_sem.at[chunk, step],
            recv_sem=recv_sem.at[chunk, step],
            device_id=cube.partner(bit),
            device_id_type=pl.DeviceIdType.MESH,
        ).start()

    each(start, 2**step, send)
    return (2**step - start) * cube.block


def reduce_kernel(
    fs, rep, kinds, partial_ref, root_ref, right_ref, gram_ref, acc, landed, held,
    load_sem, rs_send, rs_recv, ag_send, ag_recv,
):
    block = acc.shape[1] // (fs * rep)
    cube = Cube(fs, rep, block)
    chunks = len(kinds)
    dims = cube.dims
    table = orders(cube.low, cube.high)

    loads = []
    for c in range(chunks):
        load = pltpu.make_async_copy(
            partial_ref.at[:, pl.ds(c * LANES, LANES)], acc.at[c], load_sem.at[c]
        )
        load.start()
        loads.append(load)
    cube.barrier()

    offsets = []
    total = 0
    for s in range(dims):
        offsets.append(total)
        total += 2 ** (dims - 1 - s) * block

    def absorb(c, s):
        order = table[kinds[c]]
        count = 2 ** (dims - 1 - s)
        drain(landed.at[c, pl.ds(offsets[s], count * block)], rs_recv.at[c, s])
        free = order[s + 1:]

        def add(j):
            rows = cube.rows(free, j)
            got = landed[c, pl.ds(offsets[s] + j * block, block)]
            acc[c, rows] = acc[c, rows] + got

        each(0, count, add)

    def reduce_send(c, s):
        order = table[kinds[c]]
        bit = order[s]
        free = order[s + 1:]

        def send(j):
            pltpu.make_async_remote_copy(
                src_ref=acc.at[c, cube.rows(free, j, flipped=bit)],
                dst_ref=landed.at[c, pl.ds(offsets[s] + j * block, block)],
                send_sem=rs_send.at[c, s],
                recv_sem=rs_recv.at[c, s],
                device_id=cube.partner(bit),
                device_id_type=pl.DeviceIdType.MESH,
            ).start()

        each(0, 2 ** (dims - 1 - s), send)

    def finish(c):
        gathered = held[c]
        right = jnp.dot(gathered, root_ref[c], preferred_element_type=jnp.float32)
        right_ref[:, pl.ds(c * LANES, LANES)] = right.astype(jnp.bfloat16)
        gram_ref[c] = lax.dot_general(
            gathered, gathered, (((0,), (0,)), ((), ())), preferred_element_type=jnp.float32
        )

    def stage(c, s):
        if s == 0:
            loads[c].wait()
        elif s <= dims:
            absorb(c, s - 1)
        if s < dims:
            reduce_send(c, s)
            return
        order = table[kinds[c]][::-1]
        step = s - dims
        if step == 0:
            mine = cube.rows([], 0)
            held[c, mine] = acc[c, mine].astype(jnp.bfloat16)
        else:
            drain(held.at[c, pl.ds(0, 2 ** (step - 1) * block)], ag_recv.at[c, step - 1])
        if step < dims:
            gather_sends(cube, held, c, order, step, ag_send, ag_recv, False)
        else:
            finish(c)

    plan = []
    for c in range(chunks):
        late = 0 if c < 6 else 1
        rank = c if c < 3 else (c + 4 if c < 6 else c - 3)
        for s in range(2 * dims + 1):
            plan.append((s + late, rank, c, s))
    for _, _, c, s in sorted(plan):
        stage(c, s)

    for c in range(chunks):
        for s in range(dims):
            drain(acc.at[c, pl.ds(0, 2 ** (dims - 1 - s) * block)], rs_send.at[c, s])
            drain(held.at[c, pl.ds(0, 2**s * block)], ag_send.at[c, s])


def reduce_rows(partial_value, roots, fs, rep):
    height, width = partial_value.shape
    chunks = width // LANES
    kinds = (KINDS * chunks)[:chunks]
    dims = log2(fs * rep)
    block = height // (fs * rep)
    return pl.pallas_call(
        functools.partial(reduce_kernel, fs, rep, kinds),
        name="reduce_rows",
        out_shape=(
            jax.ShapeDtypeStruct((height, width), jnp.bfloat16),
            jax.ShapeDtypeStruct((chunks, LANES, LANES), jnp.float32),
        ),
        in_specs=[
            pl.BlockSpec(memory_space=pl.ANY),
            pl.BlockSpec(memory_space=pltpu.VMEM),
        ],
        out_specs=[pl.BlockSpec(memory_space=pltpu.VMEM)] * 2,
        scratch_shapes=[
            pltpu.VMEM((chunks, height, LANES), jnp.float32),
            pltpu.VMEM((chunks, height - block, LANES), jnp.float32),
            pltpu.VMEM((chunks, height, LANES), jnp.bfloat16),
            pltpu.SemaphoreType.DMA((chunks,)),
            pltpu.SemaphoreType.DMA((chunks, dims)),
            pltpu.SemaphoreType.DMA((chunks, dims)),
            pltpu.SemaphoreType.DMA((chunks, dims)),
            pltpu.SemaphoreType.DMA((chunks, dims)),
        ],
        compiler_params=pltpu.CompilerParams(
            collective_id=0, has_side_effects=True, vmem_limit_bytes=60 * 2**20
        ),
    )(partial_value, roots)


def copy_kernel(
    fs, rep, kinds, query_ref, key_ref, query_out, key_out, held, load_sem, store_sem, send_sem, recv_sem
):
    height = held.shape[1]
    block = height // (fs * rep)
    cube = Cube(fs, rep, block)
    chunks = len(kinds)
    dims = cube.dims
    table = orders(cube.low, cube.high)
    split = query_ref.shape[1] // LANES
    plane = pl.ds(pl.multiple_of(cube.f * (height // fs), height // fs), height // fs)

    def columns(c, query, key):
        ref, at = (query, c) if c < split else (key, c - split)
        return ref.at[:, pl.ds(at * LANES, LANES)]

    loads = []
    for c in range(chunks):
        load = pltpu.make_async_copy(
            columns(c, query_ref, key_ref), held.at[c, plane], load_sem.at[c]
        )
        load.start()
        loads.append(load)
    cube.barrier()

    sent = {}
    stores = []

    def stage(c, s):
        order = table[kinds[c]][::-1]
        if s == 0:
            loads[c].wait()
        else:
            drain(held.at[c, pl.ds(0, sent[c, s - 1])], recv_sem.at[c, s - 1])
        if s < dims:
            sent[c, s] = gather_sends(cube, held, c, order, s, send_sem, recv_sem, True)
        else:
            store = pltpu.make_async_copy(
                held.at[c], columns(c, query_out, key_out), store_sem.at[c]
            )
            store.start()
            stores.append(store)

    for s in range(dims + 1):
        for c in range(chunks):
            stage(c, s)
    for store in stores:
        store.wait()
    for (c, s), size in sent.items():
        drain(held.at[c, pl.ds(0, size)], send_sem.at[c, s])


def gather_copies(query, key, fs, rep):
    height = query.shape[0] * fs
    chunks = (query.shape[1] + key.shape[1]) // LANES
    kinds = (KINDS * chunks)[:chunks]
    dims = log2(fs * rep)
    return pl.pallas_call(
        functools.partial(copy_kernel, fs, rep, kinds),
        name="gather_copies",
        out_shape=(
            jax.ShapeDtypeStruct((height, query.shape[1]), jnp.bfloat16),
            jax.ShapeDtypeStruct((height, key.shape[1]), jnp.bfloat16),
        ),
        in_specs=[pl.BlockSpec(memory_space=pl.ANY)] * 2,
        out_specs=[pl.BlockSpec(memory_space=pl.ANY)] * 2,
        scratch_shapes=[
            pltpu.VMEM((chunks, height, LANES), jnp.bfloat16),
            pltpu.SemaphoreType.DMA((chunks,)),
            pltpu.SemaphoreType.DMA((chunks,)),
            pltpu.SemaphoreType.DMA((chunks, dims)),
            pltpu.SemaphoreType.DMA((chunks, dims)),
        ],
        compiler_params=pltpu.CompilerParams(
            collective_id=1, has_side_effects=True, vmem_limit_bytes=32 * 2**20
        ),
    )(query, key)


def pair_roots(query_head_root, key_head_root):
    roots = jnp.concatenate([query_head_root, key_head_root], axis=0)
    roots = roots.reshape(-1, 2, HEAD_DIM, HEAD_DIM)
    zero = jnp.zeros_like(roots[:, 0])
    upper = jnp.concatenate([roots[:, 0], zero], axis=2)
    lower = jnp.concatenate([zero, roots[:, 1]], axis=2)
    return jnp.concatenate([upper, lower], axis=1)


def unpair(grams):
    first = grams[:, :HEAD_DIM, :HEAD_DIM]
    second = grams[:, HEAD_DIM:, HEAD_DIM:]
    return jnp.stack([first, second], axis=1).reshape(-1, HEAD_DIM, HEAD_DIM)


def shards(
    fs,
    rep,
    saved_input,
    query_cotangent,
    key_cotangent,
    query_weight,
    key_weight,
    query_moment,
    key_moment,
    query_row_root,
    key_row_root,
    query_head_root,
    key_head_root,
    query_head_stat,
    key_head_stat,
):
    height = saved_input.shape[1]
    query_width = query_cotangent.shape[1]
    query_heads = query_head_root.shape[0]
    cotangents = jnp.concatenate([query_cotangent, key_cotangent], axis=1)
    partial_value = lax.dot_general(
        saved_input, cotangents, (((0,), (0,)), ((), ())), preferred_element_type=jnp.float32
    )
    right, grams = reduce_rows(partial_value, pair_roots(query_head_root, key_head_root), fs, rep)
    grams = unpair(grams)
    query_stat_next = (
        STAT_DECAY * query_head_stat + (1.0 - STAT_DECAY) * grams[:query_heads] / height
    )
    key_stat_next = STAT_DECAY * key_head_stat + (1.0 - STAT_DECAY) * grams[query_heads:] / height
    query_pre = jnp.dot(
        query_row_root, right[:, :query_width], preferred_element_type=jnp.float32
    )
    key_pre = jnp.dot(key_row_root, right[:, query_width:], preferred_element_type=jnp.float32)
    query_moment_next = MOMENT_DECAY * query_moment + (1.0 - MOMENT_DECAY) * query_pre
    key_moment_next = MOMENT_DECAY * key_moment + (1.0 - MOMENT_DECAY) * key_pre
    query_wsq, query_msq, key_wsq, key_msq = lax.psum(
        (
            jnp.sum(query_weight * query_weight),
            jnp.sum(query_moment_next * query_moment_next),
            jnp.sum(key_weight * key_weight),
            jnp.sum(key_moment_next * key_moment_next),
        ),
        ("fs", "tp"),
    )
    query_step = (
        LEARN_RATE * (jnp.sqrt(query_wsq) / jnp.sqrt(query_msq + EPSILON)) * query_moment_next
    )
    key_step = LEARN_RATE * (jnp.sqrt(key_wsq) / jnp.sqrt(key_msq + EPSILON)) * key_moment_next
    query_next = query_weight - query_step
    key_next = key_weight - key_step
    query_copy, key_copy = gather_copies(
        query_next.astype(jnp.bfloat16), key_next.astype(jnp.bfloat16), fs, rep
    )
    return (
        query_step,
        key_step,
        query_next,
        key_next,
        query_copy,
        key_copy,
        query_moment_next,
        key_moment_next,
        query_stat_next,
        key_stat_next,
    )


def solution(mesh):
    in_specs = (
        P(("fs", "rep"), None),
        P(("fs", "rep"), "tp"),
        P(("fs", "rep"), "tp"),
        P("fs", "tp"),
        P("fs", "tp"),
        P("fs", "tp"),
        P("fs", "tp"),
        P("fs", None),
        P("fs", None),
        P("tp", None, None),
        P("tp", None, None),
        P("tp", None, None),
        P("tp", None, None),
    )
    out_specs = (
        P("fs", "tp"),
        P("fs", "tp"),
        P("fs", "tp"),
        P("fs", "tp"),
        P(None, "tp"),
        P(None, "tp"),
        P("fs", "tp"),
        P("fs", "tp"),
        P("tp", None, None),
        P("tp", None, None),
    )
    body = functools.partial(shards, mesh.shape["fs"], mesh.shape["rep"])
    return jax.shard_map(body, mesh=mesh, in_specs=in_specs, out_specs=out_specs, check_vma=False)
```

```python
import functools

import jax
import jax.numpy as jnp
from jax import lax
from jax.experimental import pallas as pl
from jax.experimental.pallas import tpu as pltpu
from jax.sharding import PartitionSpec as P

HEAD_DIM = 64
LANES = 128

MOMENT_DECAY = 0.8
STAT_DECAY = 0.5
LEARN_RATE = 0.1
EPSILON = 1e-06


def log2(n):
    return n.bit_length() - 1


class Cube:
    def __init__(self, fs, rep, block):
        self.fs, self.rep, self.block = fs, rep, block
        self.low, self.high = log2(rep), log2(fs)
        self.dims = self.low + self.high
        f, r = lax.axis_index("fs"), lax.axis_index("rep")
        self.f, self.r = f, r
        self.bits = [(r // 2**k) % 2 for k in range(self.low)]
        self.bits += [(f // 2**k) % 2 for k in range(self.high)]
        self.me = f * rep + r

    def partner(self, bit):
        flip = 1 - 2 * self.bits[bit]
        if bit < self.low:
            return {"rep": self.r + flip * 2**bit}
        return {"fs": self.f + flip * 2 ** (bit - self.low)}

    def rows(self, free, j, flipped=None):
        index = self.me
        for k, bit in enumerate(free):
            index = index + ((j // 2**k) % 2) * ((1 - 2 * self.bits[bit]) * 2**bit)
        if flipped is not None:
            index = index + (1 - 2 * self.bits[flipped]) * 2**flipped
        return pl.ds(pl.multiple_of(index * self.block, self.block), self.block)

    def barrier(self):
        barrier = pltpu.get_barrier_semaphore()
        for bit in range(self.dims):
            pl.semaphore_signal(
                barrier, inc=1, device_id=self.partner(bit), device_id_type=pl.DeviceIdType.MESH
            )
        pl.semaphore_wait(barrier, self.dims)


def each(start, stop, body):
    if stop - start <= 8:
        for j in range(start, stop):
            body(j)
    else:
        lax.fori_loop(start, stop, lambda j, _: (body(j), 0)[1], 0)


def orders(low, high):
    rep_bits, fs_bits = list(range(low)), list(range(low, low + high))
    near, far = fs_bits[:1], fs_bits[1:]
    return {
        "a": rep_bits + near + far,
        "b": rep_bits[::-1] + near + far,
        "c": near + rep_bits + far,
        "d": near + rep_bits[::-1] + far,
    }


KINDS = "abcdababab"


def wavefront(chunks, last):
    plan = []
    for c in range(chunks):
        delay = 2 * min(2, (max(c - 1, 0) * 3) // max(chunks - 1, 1))
        for s in range(last + 1):
            turn = 0 if s == 0 else (2 if s == last else 1)
            plan.append((s + delay, turn, c, s))
    return [(c, s) for _, _, c, s in sorted(plan)]


def drain(ref, sem):
    pltpu.make_async_copy(ref, ref, sem).wait()


def gather_sends(cube, held, chunk, order, step, send_sem, recv_sem, known_plane):
    bit = order[step]
    free = sorted(order[:step])
    start = 0
    if known_plane and bit < cube.low:
        start = 2 ** len([b for b in free if b < cube.low])

    def send(j):
        rows = cube.rows(free, j)
        pltpu.make_async_remote_copy(
            src_ref=held.at[chunk, rows],
            dst_ref=held.at[chunk, rows],
            send_sem=send_sem.at[chunk, step],
            recv_sem=recv_sem.at[chunk, step],
            device_id=cube.partner(bit),
            device_id_type=pl.DeviceIdType.MESH,
        ).start()

    each(start, 2**step, send)
    return (2**step - start) * cube.block


def reduce_kernel(
    fs, rep, kinds, partial_ref, root_ref, right_ref, gram_ref, acc, landed, held,
    load_sem, rs_send, rs_recv, ag_send, ag_recv,
):
    block = acc.shape[1] // (fs * rep)
    cube = Cube(fs, rep, block)
    chunks = len(kinds)
    dims = cube.dims
    table = orders(cube.low, cube.high)

    loads = []
    for c in range(chunks):
        load = pltpu.make_async_copy(
            partial_ref.at[:, pl.ds(c * LANES, LANES)], acc.at[c], load_sem.at[c]
        )
        load.start()
        loads.append(load)
    cube.barrier()

    offsets = []
    total = 0
    for s in range(dims):
        offsets.append(total)
        total += 2 ** (dims - 1 - s) * block

    def absorb(c, s):
        order = table[kinds[c]]
        count = 2 ** (dims - 1 - s)
        drain(landed.at[c, pl.ds(offsets[s], count * block)], rs_recv.at[c, s])
        free = order[s + 1:]

        def add(j):
            rows = cube.rows(free, j)
            got = landed[c, pl.ds(offsets[s] + j * block, block)]
            acc[c, rows] = acc[c, rows] + got

        each(0, count, add)

    def reduce_send(c, s):
        order = table[kinds[c]]
        bit = order[s]
        free = order[s + 1:]

        def send(j):
            pltpu.make_async_remote_copy(
                src_ref=acc.at[c, cube.rows(free, j, flipped=bit)],
                dst_ref=landed.at[c, pl.ds(offsets[s] + j * block, block)],
                send_sem=rs_send.at[c, s],
                recv_sem=rs_recv.at[c, s],
                device_id=cube.partner(bit),
                device_id_type=pl.DeviceIdType.MESH,
            ).start()

        each(0, 2 ** (dims - 1 - s), send)

    def finish(c):
        gathered = held[c]
        right = jnp.dot(gathered, root_ref[c], preferred_element_type=jnp.float32)
        right_ref[:, pl.ds(c * LANES, LANES)] = right.astype(jnp.bfloat16)
        gram_ref[c] = lax.dot_general(
            gathered, gathered, (((0,), (0,)), ((), ())), preferred_element_type=jnp.float32
        )

    def stage(c, s):
        if s == 0:
            loads[c].wait()
        elif s <= dims:
            absorb(c, s - 1)
        if s < dims:
            reduce_send(c, s)
            return
        order = table[kinds[c]][::-1]
        step = s - dims
        if step == 0:
            mine = cube.rows([], 0)
            held[c, mine] = acc[c, mine].astype(jnp.bfloat16)
        else:
            drain(held.at[c, pl.ds(0, 2 ** (step - 1) * block)], ag_recv.at[c, step - 1])
        if step < dims:
            gather_sends(cube, held, c, order, step, ag_send, ag_recv, False)
        else:
            finish(c)

    for c, s in wavefront(chunks, 2 * dims):
        stage(c, s)

    for c in range(chunks):
        for s in range(dims):
            drain(acc.at[c, pl.ds(0, 2 ** (dims - 1 - s) * block)], rs_send.at[c, s])
            drain(held.at[c, pl.ds(0, 2**s * block)], ag_send.at[c, s])


def reduce_rows(partial_value, roots, fs, rep):
    height, width = partial_value.shape
    chunks = width // LANES
    kinds = (KINDS * chunks)[:chunks]
    dims = log2(fs * rep)
    block = height // (fs * rep)
    return pl.pallas_call(
        functools.partial(reduce_kernel, fs, rep, kinds),
        name="reduce_rows",
        out_shape=(
            jax.ShapeDtypeStruct((height, width), jnp.bfloat16),
            jax.ShapeDtypeStruct((chunks, LANES, LANES), jnp.float32),
        ),
        in_specs=[
            pl.BlockSpec(memory_space=pl.ANY),
            pl.BlockSpec(memory_space=pltpu.VMEM),
        ],
        out_specs=[pl.BlockSpec(memory_space=pltpu.VMEM)] * 2,
        scratch_shapes=[
            pltpu.VMEM((chunks, height, LANES), jnp.float32),
            pltpu.VMEM((chunks, height - block, LANES), jnp.float32),
            pltpu.VMEM((chunks, height, LANES), jnp.bfloat16),
            pltpu.SemaphoreType.DMA((chunks,)),
            pltpu.SemaphoreType.DMA((chunks, dims)),
            pltpu.SemaphoreType.DMA((chunks, dims)),
            pltpu.SemaphoreType.DMA((chunks, dims)),
            pltpu.SemaphoreType.DMA((chunks, dims)),
        ],
        compiler_params=pltpu.CompilerParams(
            collective_id=0, has_side_effects=True, vmem_limit_bytes=60 * 2**20
        ),
    )(partial_value, roots)


def copy_kernel(
    fs, rep, kinds, query_ref, key_ref, query_out, key_out, held, load_sem, store_sem, send_sem, recv_sem
):
    height = held.shape[1]
    block = height // (fs * rep)
    cube = Cube(fs, rep, block)
    chunks = len(kinds)
    dims = cube.dims
    table = orders(cube.low, cube.high)
    split = query_ref.shape[1] // LANES
    plane = pl.ds(pl.multiple_of(cube.f * (height // fs), height // fs), height // fs)

    def columns(c, query, key):
        ref, at = (query, c) if c < split else (key, c - split)
        return ref.at[:, pl.ds(at * LANES, LANES)]

    loads = []
    for c in range(chunks):
        load = pltpu.make_async_copy(
            columns(c, query_ref, key_ref), held.at[c, plane], load_sem.at[c]
        )
        load.start()
        loads.append(load)
    cube.barrier()

    sent = {}
    stores = []

    def stage(c, s):
        order = table[kinds[c]][::-1]
        if s == 0:
            loads[c].wait()
        else:
            drain(held.at[c, pl.ds(0, sent[c, s - 1])], recv_sem.at[c, s - 1])
        if s < dims:
            sent[c, s] = gather_sends(cube, held, c, order, s, send_sem, recv_sem, True)
        else:
            store = pltpu.make_async_copy(
                held.at[c], columns(c, query_out, key_out), store_sem.at[c]
            )
            store.start()
            stores.append(store)

    for c, s in wavefront(chunks, dims):
        stage(c, s)
    for store in stores:
        store.wait()
    for (c, s), size in sent.items():
        drain(held.at[c, pl.ds(0, size)], send_sem.at[c, s])


def gather_copies(query, key, fs, rep):
    height = query.shape[0] * fs
    chunks = (query.shape[1] + key.shape[1]) // LANES
    kinds = (KINDS * chunks)[:chunks]
    dims = log2(fs * rep)
    return pl.pallas_call(
        functools.partial(copy_kernel, fs, rep, kinds),
        name="gather_copies",
        out_shape=(
            jax.ShapeDtypeStruct((height, query.shape[1]), jnp.bfloat16),
            jax.ShapeDtypeStruct((height, key.shape[1]), jnp.bfloat16),
        ),
        in_specs=[pl.BlockSpec(memory_space=pl.ANY)] * 2,
        out_specs=[pl.BlockSpec(memory_space=pl.ANY)] * 2,
        scratch_shapes=[
            pltpu.VMEM((chunks, height, LANES), jnp.bfloat16),
            pltpu.SemaphoreType.DMA((chunks,)),
            pltpu.SemaphoreType.DMA((chunks,)),
            pltpu.SemaphoreType.DMA((chunks, dims)),
            pltpu.SemaphoreType.DMA((chunks, dims)),
        ],
        compiler_params=pltpu.CompilerParams(
            collective_id=1, has_side_effects=True, vmem_limit_bytes=32 * 2**20
        ),
    )(query, key)


def pair_roots(query_head_root, key_head_root):
    roots = jnp.concatenate([query_head_root, key_head_root], axis=0)
    roots = roots.reshape(-1, 2, HEAD_DIM, HEAD_DIM)
    zero = jnp.zeros_like(roots[:, 0])
    upper = jnp.concatenate([roots[:, 0], zero], axis=2)
    lower = jnp.concatenate([zero, roots[:, 1]], axis=2)
    return jnp.concatenate([upper, lower], axis=1)


def unpair(grams):
    first = grams[:, :HEAD_DIM, :HEAD_DIM]
    second = grams[:, HEAD_DIM:, HEAD_DIM:]
    return jnp.stack([first, second], axis=1).reshape(-1, HEAD_DIM, HEAD_DIM)


def shards(
    fs,
    rep,
    saved_input,
    query_cotangent,
    key_cotangent,
    query_weight,
    key_weight,
    query_moment,
    key_moment,
    query_row_root,
    key_row_root,
    query_head_root,
    key_head_root,
    query_head_stat,
    key_head_stat,
):
    height = saved_input.shape[1]
    query_width = query_cotangent.shape[1]
    query_heads = query_head_root.shape[0]
    cotangents = jnp.concatenate([query_cotangent, key_cotangent], axis=1)
    partial_value = lax.dot_general(
        saved_input, cotangents, (((0,), (0,)), ((), ())), preferred_element_type=jnp.float32
    )
    right, grams = reduce_rows(partial_value, pair_roots(query_head_root, key_head_root), fs, rep)
    grams = unpair(grams)
    query_stat_next = (
        STAT_DECAY * query_head_stat + (1.0 - STAT_DECAY) * grams[:query_heads] / height
    )
    key_stat_next = STAT_DECAY * key_head_stat + (1.0 - STAT_DECAY) * grams[query_heads:] / height
    query_pre = jnp.dot(
        query_row_root, right[:, :query_width], preferred_element_type=jnp.float32
    )
    key_pre = jnp.dot(key_row_root, right[:, query_width:], preferred_element_type=jnp.float32)
    query_moment_next = MOMENT_DECAY * query_moment + (1.0 - MOMENT_DECAY) * query_pre
    key_moment_next = MOMENT_DECAY * key_moment + (1.0 - MOMENT_DECAY) * key_pre
    query_wsq, query_msq, key_wsq, key_msq = lax.psum(
        (
            jnp.sum(query_weight * query_weight),
            jnp.sum(query_moment_next * query_moment_next),
            jnp.sum(key_weight * key_weight),
            jnp.sum(key_moment_next * key_moment_next),
        ),
        ("fs", "tp"),
    )
    query_step = (
        LEARN_RATE * (jnp.sqrt(query_wsq) / jnp.sqrt(query_msq + EPSILON)) * query_moment_next
    )
    key_step = LEARN_RATE * (jnp.sqrt(key_wsq) / jnp.sqrt(key_msq + EPSILON)) * key_moment_next
    query_next = query_weight - query_step
    key_next = key_weight - key_step
    query_copy, key_copy = gather_copies(
        query_next.astype(jnp.bfloat16), key_next.astype(jnp.bfloat16), fs, rep
    )
    return (
        query_step,
        key_step,
        query_next,
        key_next,
        query_copy,
        key_copy,
        query_moment_next,
        key_moment_next,
        query_stat_next,
        key_stat_next,
    )


def solution(mesh):
    in_specs = (
        P(("fs", "rep"), None),
        P(("fs", "rep"), "tp"),
        P(("fs", "rep"), "tp"),
        P("fs", "tp"),
        P("fs", "tp"),
        P("fs", "tp"),
        P("fs", "tp"),
        P("fs", None),
        P("fs", None),
        P("tp", None, None),
        P("tp", None, None),
        P("tp", None, None),
        P("tp", None, None),
    )
    out_specs = (
        P("fs", "tp"),
        P("fs", "tp"),
        P("fs", "tp"),
        P("fs", "tp"),
        P(None, "tp"),
        P(None, "tp"),
        P("fs", "tp"),
        P("fs", "tp"),
        P("tp", None, None),
        P("tp", None, None),
    )
    body = functools.partial(shards, mesh.shape["fs"], mesh.shape["rep"])
    return jax.shard_map(body, mesh=mesh, in_specs=in_specs, out_specs=out_specs, check_vma=False)
```
